32 devices in a mesh: grp: 2 (over y), sp: 8 (over z, core), tp: 2 (over x).
Axes of the slice: x: 2, y: 2, z: 4, core: 2. Of those that a mesh axis runs over, the one named last changes fastest.
Arguments:
- query_plain: bfloat16 [2560, 1024], P(('grp', 'sp'), 'tp'), parts along dimension 0, may hold values from -6 to 6
- query_turn: bfloat16 [2560, 512], P(('grp', 'sp'), 'tp'), parts along dimension 0, may hold values from -40 to 40, as said below
- latent: bfloat16 [2560, 512], P(('grp', 'sp')), parts along dimension 0, may hold values from -6 to 6
- key_turn: bfloat16 [2560, 64], P(('grp', 'sp')), parts along dimension 0, may hold values from -40 to 40, as said below
- latent_norm_scale: bfloat16 [512], replicated, may hold values from 0.099609375 to 1.8984375
- plain_key_matrix: bfloat16 [512, 1024], P(None, 'tp'), may hold values from -0.25 to 0.25
- value_matrix: bfloat16 [512, 1024], P(None, 'tp'), may hold values from -0.25 to 0.25
- residual: bfloat16 [2560, 2048], P(('grp', 'sp', 'tp')), parts along dimension 0, may hold values from -6 to 6
- out_weight: bfloat16 [1024, 2048], replicated, may hold values from -6 to 6
- ffn_gain: bfloat16 [2048], replicated, may hold values from 0.099609375 to 1.8984375
- gate_weight: bfloat16 [8, 2048, 1024], P('sp', None, 'tp'), may hold values from -1 to 1
- up_weight: bfloat16 [8, 2048, 1024], P('sp', None, 'tp'), may hold values from -1 to 1
- down_weight: bfloat16 [8, 1024, 2048], P('sp', 'tp'), may hold values from -0.0625 to 0.0625
- routes: int32 [2560, 4], P(('grp', 'sp', 'tp')), parts along dimension 0, may hold values from 0 to 7, all different within a row; in each aligned block of 80 rows (0 to 79, 80 to 159, ...) at most 60 rows name the same one
- route_weights: float32 [2560, 4], P(('grp', 'sp', 'tp')), parts along dimension 0, may hold values from 0.1 to 0.6
Outputs:
- mixed: bfloat16 [2560, 2048], P(('grp', 'sp', 'tp')), parts along dimension 0
The draws below stay inside these ranges and needn't reach their ends.
There are 2 independent parts, one for each index of `grp`. The reference program is written for one: setup_inputs(seed, part) draws one part's arguments, and reference() takes and returns one part's arrays. A program takes and returns all parts, laid end to end along the dimension named above; an argument that names none is the same for every part. Nothing has to cross between parts.
Inputs may be any that keep to these rules, and one draw needn't show every extreme that they name: `query_turn`: in the hidden draw some rows are large. `key_turn`: in the hidden draw some rows are large. `routes`: each row names 4 different experts. In each aligned block of 80 rows (the rows of one device) no expert is named more than 60 times, a bound that some block reaches.
All inputs are finite; a program needn't handle non-finite values.
Results may differ from the reference program's by a relative error of at most 0.015.
Values may be sent and summed in bfloat16 or wider, within the bound.
A program may use at most 128 MiB of HBM per device.

```python
import math
import jax
import jax.numpy as jnp
import numpy as np
from jax import lax

D = 2048
ATTENTION_HEADS = 8
PLAIN_HEAD_WIDTH = 128
QK_ROPE = 64
VALUE_WIDTH = 128
LATENT_WIDTH = 512
D_EXPERT = 1024
TOP = 4
GRID_W = 64
ROWS_DEV = 80
SEQUENCE_TOKENS = 1280
EXPERTS = 8
CAP = 60
N_SP = 8
N_TP = 2


def draw_query_turn(key, part):
    base = jnp.clip(jax.random.normal(jax.random.fold_in(key, 1), (SEQUENCE_TOKENS, ATTENTION_HEADS * QK_ROPE), jnp.float32), -6.0, 6.0)
    return base.astype(jnp.bfloat16)


def draw_key_turn(key, part):
    base = jnp.clip(jax.random.normal(jax.random.fold_in(key, 2), (SEQUENCE_TOKENS, QK_ROPE), jnp.float32), -6.0, 6.0)
    return base.astype(jnp.bfloat16)


def block_scale(own_key, extent, cuts, least, high):
    loudness, own = 1.0, jax.random.fold_in(own_key, 6)
    for dim, shards_of in cuts:
        steps = jnp.exp(jax.random.uniform(jax.random.fold_in(own, dim), (shards_of,), jnp.float32, least / len(cuts), high / len(cuts)))
        loudness = loudness * jnp.repeat(steps, extent[dim] // shards_of).reshape([-1 if axis == dim else 1 for axis in range(len(extent))])
    return loudness


def shared_out(stream_key, own, number, rows, count, top, reach, skew):
    ranking = jax.random.permutation(stream_key, count)
    crowded, common = shares(count, rows * top, reach, skew, True), shares(count, rows * top, reach, skew, False)
    places = jnp.arange(count)

    def named(sizes, offset_by):
        used = int((sizes > 0).sum())
        fixed = max(1, used // 4)
        passed = fixed + (places - fixed + offset_by * (used - fixed)) % max(1, count - fixed)
        return jnp.zeros((count,), jnp.int32).at[ranking[jnp.where(places < fixed, places, passed)]].set(jnp.asarray(sizes, jnp.int32))

    sizes = jnp.where(number % 4 == 0, named(crowded, number // 4), named(common, number - number // 4 - 1))
    mixed = jax.random.permutation(jax.random.fold_in(own, 3), count)
    source_of, sink = mixed[0:count // 2 * 2:2], mixed[1:count // 2 * 2:2]
    slack = jnp.minimum(sizes[source_of] - 1, reach - sizes[sink]) // 2
    slack = jnp.where((source_of == ranking[0]) | (sink == ranking[0]) | (sizes[sink] == 0), 0, jnp.maximum(slack, 0))
    passed = jax.random.randint(jax.random.fold_in(own, 4), (count // 2,), 0, 1 << 20) % (slack + 1)
    sizes = sizes.at[source_of].add(-passed).at[sink].add(passed)
    members = jnp.searchsorted(jnp.cumsum(sizes), jnp.arange(rows * top), side="right").astype(jnp.int32)
    grid = members.reshape(top, rows).T
    grid = grid[jax.random.permutation(jax.random.fold_in(own, 1), rows)]
    offset_by = jax.random.randint(jax.random.fold_in(own, 2), (rows, 1), 0, top)
    return jnp.take_along_axis(grid, (jnp.arange(top)[None, :] + offset_by) % top, axis=1)


def shares(count, total, most, lean, full):
    loads = [(1 << 20) // math.isqrt(standing ** lean) + 1 for standing in range(1, count + 1)]
    largest = most if full else min(most, max(-(-total // count), total * loads[0] // sum(loads)))
    least = 1 if total - largest >= count - 1 else 0
    given, surplus = [largest] + [least] * (count - 1), total - largest - least * (count - 1)
    while surplus > 0:
        candidates = [i for i in range(1, count) if given[i] < largest] or [i for i in range(1, count) if given[i] < most]
        whole, budget = sum([loads[i] for i in candidates]), surplus
        for i in candidates:
            more = min(most - given[i], max(1, budget * loads[i] // whole), surplus)
            given[i] = given[i] + more
            surplus = surplus - more
    return np.array(given)


def scatter_about(own_key, dims, scale, bound, shards=(), kind=jnp.bfloat16):
    drawn = jax.random.normal(own_key, dims, jnp.float32) * scale
    if len(shards) > 0:
        drawn = block_scale(own_key, dims, shards, -0.22, 0.18) * drawn
    return jnp.clip(drawn, min=-bound, max=bound).astype(kind)


def setup_inputs(seed: int = 0, part: int = 0) -> dict:
    arg_keys = jax.random.split(jax.random.key(seed), 16)
    part_keys = jax.random.split(jax.random.fold_in(arg_keys[15], part), 16)
    query_plain = scatter_about(part_keys[0], (SEQUENCE_TOKENS, ATTENTION_HEADS * PLAIN_HEAD_WIDTH), 1.0, 6.0, ((0, 8), (1, 2)))
    query_turn = draw_query_turn(jax.random.fold_in(jax.random.fold_in(arg_keys[15], part), 71), part)
    latent = scatter_about(part_keys[2], (SEQUENCE_TOKENS, LATENT_WIDTH), 1.0, 6.0, ((0, 8),))
    key_turn = draw_key_turn(jax.random.fold_in(jax.random.fold_in(arg_keys[15], part), 71), part)
    latent_norm_scale = jnp.clip(1.0 + 0.18 * jax.random.normal(arg_keys[4], (LATENT_WIDTH,), jnp.float32), 0.099609375, 1.8984375).astype(jnp.bfloat16)
    plain_key_matrix = scatter_about(arg_keys[5], (LATENT_WIDTH, ATTENTION_HEADS * PLAIN_HEAD_WIDTH), LATENT_WIDTH ** -0.5, 0.25, ((1, 2),))
    value_matrix = scatter_about(arg_keys[6], (LATENT_WIDTH, ATTENTION_HEADS * VALUE_WIDTH), LATENT_WIDTH ** -0.5, 0.25, ((1, 2),))
    residual = scatter_about(part_keys[7], (SEQUENCE_TOKENS, D), 1.0, 6.0, ((0, 16),))
    out_weight = scatter_about(arg_keys[8], (ATTENTION_HEADS * VALUE_WIDTH, D), (16 * (ATTENTION_HEADS * VALUE_WIDTH) ** -0.5), 6.0)
    ffn_gain = jnp.clip(1.0 + 0.18 * jax.random.normal(arg_keys[9], (D,), jnp.float32), 0.099609375, 1.8984375).astype(jnp.bfloat16)
    gate_weight = scatter_about(arg_keys[10], (EXPERTS, D, D_EXPERT), (3 * D ** -0.5), 1.0, ((0, 8), (2, 2)))
    up_weight = scatter_about(arg_keys[11], (EXPERTS, D, D_EXPERT), (3 * D ** -0.5), 1.0, ((0, 8), (2, 2)))
    down_weight = scatter_about(arg_keys[12], (EXPERTS, D_EXPERT, D), (0.15 * D_EXPERT ** -0.5), 0.0625, ((0, 8), (1, 2)))
    routes_keys = jax.random.split(jax.random.fold_in(part_keys[13], 1), SEQUENCE_TOKENS // ROWS_DEV)
    routes_turns = jax.random.permutation(jax.random.fold_in(part_keys[13], 3), SEQUENCE_TOKENS // ROWS_DEV)
    routes = jax.vmap(lambda own, number: shared_out(jax.random.fold_in(part_keys[13], 2), own, number, ROWS_DEV, EXPERTS, TOP, CAP, 1))(routes_keys, routes_turns).reshape((SEQUENCE_TOKENS, TOP))
    route_weights = jnp.clip(0.1 + 0.5 * jax.random.uniform(part_keys[14], (SEQUENCE_TOKENS, TOP), jnp.float32) ** block_scale(part_keys[14], (SEQUENCE_TOKENS, TOP), ((0, 16),), -0.2, 0.2), 0.1, 0.6)
    return dict(query_plain=query_plain, query_turn=query_turn, latent=latent, key_turn=key_turn, latent_norm_scale=latent_norm_scale, plain_key_matrix=plain_key_matrix, value_matrix=value_matrix, residual=residual, out_weight=out_weight, ffn_gain=ffn_gain, gate_weight=gate_weight, up_weight=up_weight, down_weight=down_weight, routes=routes, route_weights=route_weights)


theta = 10000.0
eps = 1e-06
limit = 7.0
slope = 1.702

def turn(vector, row_shift, col_shift):
    width = vector.shape[-1]
    count = width // 4
    half = width // 2
    freqs = theta ** (-jnp.arange(count, dtype=jnp.float32) / count)
    extra = (1,) * (vector.ndim - 2)
    pieces = []
    for portion, shift in ((vector[..., :half], row_shift), (vector[..., half:], col_shift)):
        angle = (shift.astype(jnp.float32)[:, None] * freqs[None, :]).reshape((shift.shape[0],) + extra + (count,))
        lower = portion[..., :count]
        upper = portion[..., count:]
        pieces.append(jnp.concatenate([lower * jnp.cos(angle) - upper * jnp.sin(angle), lower * jnp.sin(angle) + upper * jnp.cos(angle)], axis=-1))
    return jnp.concatenate(pieces, axis=-1)

def norm_scale(values, gain):
    wide = values.astype(jnp.float32)
    return wide * lax.rsqrt(lax.optimization_barrier(jnp.mean(wide * wide, axis=-1, keepdims=True)) + eps) * gain.astype(jnp.float32)

def expert_apply(operands):
    rows, gate_w, up_w, down_w = operands
    gate_pre = jnp.minimum(jnp.dot(rows, gate_w, preferred_element_type=jnp.float32), limit)
    up_pre = jnp.clip(jnp.dot(rows, up_w, preferred_element_type=jnp.float32), -limit, limit)
    active = ((up_pre + 1.0) * gate_pre * jax.nn.sigmoid(slope * gate_pre)).astype(jnp.bfloat16)
    piece = down_w.shape[0] // N_TP
    groups = jnp.einsum('rnp,npd->nrd', active.reshape(rows.shape[0], N_TP, piece).astype(jnp.float32), down_w.reshape(N_TP, piece, down_w.shape[1]).astype(jnp.float32))
    rounded = lax.optimization_barrier(groups.astype(jnp.bfloat16))
    return lax.optimization_barrier(jnp.sum(rounded.astype(jnp.float32), axis=0)).astype(jnp.bfloat16)

def reference(query_plain, query_turn, latent, key_turn, latent_norm_scale, plain_key_matrix, value_matrix, residual, out_weight, ffn_gain, gate_weight, up_weight, down_weight, routes, route_weights):
    place = jnp.arange(SEQUENCE_TOKENS, dtype=jnp.int32)
    grid_row = place // GRID_W
    grid_col = place % GRID_W
    normed_latent = norm_scale(latent, latent_norm_scale).astype(jnp.bfloat16)
    key_plain = jnp.dot(normed_latent, plain_key_matrix, preferred_element_type=jnp.float32).astype(jnp.bfloat16)
    values = jnp.dot(normed_latent, value_matrix, preferred_element_type=jnp.float32).astype(jnp.bfloat16)
    key_rot = turn(key_turn.astype(jnp.float32), grid_row, grid_col).astype(jnp.bfloat16)
    query_rot = turn(query_turn.astype(jnp.float32).reshape(SEQUENCE_TOKENS, ATTENTION_HEADS, QK_ROPE), grid_row, grid_col).astype(jnp.bfloat16)
    plain_heads = jnp.moveaxis(query_plain.reshape(SEQUENCE_TOKENS, ATTENTION_HEADS, PLAIN_HEAD_WIDTH), 1, 0)
    rot_heads = jnp.moveaxis(query_rot, 1, 0)
    key_heads = jnp.moveaxis(key_plain.reshape(SEQUENCE_TOKENS, ATTENTION_HEADS, PLAIN_HEAD_WIDTH), 1, 0)
    value_heads = jnp.moveaxis(values.reshape(SEQUENCE_TOKENS, ATTENTION_HEADS, VALUE_WIDTH), 1, 0)
    scale = (PLAIN_HEAD_WIDTH + QK_ROPE) ** (-0.5)
    block = math.gcd(SEQUENCE_TOKENS, 512)

    def one_head(operands):
        head_plain, head_rot, head_keys, head_values = operands

        def one_block(start):
            block_plain = lax.dynamic_slice_in_dim(head_plain, start, block, 0)
            block_rot = lax.dynamic_slice_in_dim(head_rot, start, block, 0)
            scores = (jnp.einsum('qd,kd->qk', block_plain, head_keys, preferred_element_type=jnp.float32) + jnp.einsum('qd,kd->qk', block_rot, key_rot, preferred_element_type=jnp.float32)) * scale
            peak = lax.optimization_barrier(jnp.max(scores, axis=1, keepdims=True))
            weights = jnp.exp(scores - peak)
            summed = jnp.dot(weights.astype(jnp.bfloat16), head_values, preferred_element_type=jnp.float32)
            return (summed / lax.optimization_barrier(jnp.sum(weights, axis=1, keepdims=True))).astype(jnp.bfloat16)
        starts = jnp.arange(SEQUENCE_TOKENS // block, dtype=jnp.int32) * block
        return lax.map(one_block, starts).reshape(SEQUENCE_TOKENS, VALUE_WIDTH)
    attended = lax.map(one_head, (plain_heads, rot_heads, key_heads, value_heads))
    attended = jnp.moveaxis(attended, 0, 1).reshape(SEQUENCE_TOKENS, ATTENTION_HEADS * VALUE_WIDTH)
    hidden = (residual.astype(jnp.float32) + jnp.dot(attended, out_weight, preferred_element_type=jnp.float32)).astype(jnp.bfloat16)
    normed = norm_scale(hidden, ffn_gain).astype(jnp.bfloat16)
    blocks = N_SP * N_TP
    per_block = routes.reshape(blocks, ROWS_DEV * TOP)
    marks = (per_block[..., None] == jnp.arange(EXPERTS, dtype=jnp.int32)).astype(jnp.int32)
    earlier = jnp.cumsum(marks, axis=1, dtype=jnp.int32) - marks
    slots = lax.optimization_barrier(jnp.sum(earlier * marks, axis=2, dtype=jnp.int32))
    target = ((per_block * blocks + jnp.arange(blocks, dtype=jnp.int32)[:, None]) * CAP + slots).reshape(SEQUENCE_TOKENS * TOP)
    copies = jnp.repeat(normed, TOP, axis=0)
    buffer = jnp.zeros((EXPERTS * blocks * CAP, D), jnp.bfloat16).at[target].set(copies)
    results = lax.map(expert_apply, (buffer.reshape(EXPERTS, blocks * CAP, D), gate_weight, up_weight, down_weight))
    results = results.reshape(EXPERTS * blocks * CAP, D)
    picked = results[target].reshape(SEQUENCE_TOKENS, TOP, D).astype(jnp.float32)
    return (hidden.astype(jnp.float32) + lax.optimization_barrier(jnp.sum(route_weights[..., None] * picked, axis=1))).astype(jnp.bfloat16)
```

```python
import jax
import jax.numpy as jnp
from jax import lax
from jax.sharding import PartitionSpec as P

PLAIN_HEAD_WIDTH = 128
QK_ROPE = 64
VALUE_WIDTH = 128
GRID_W = 64


theta = 10000.0
eps = 1e-06
limit = 7.0
slope = 1.702


def turn(vector, row_shift, col_shift):
    width = vector.shape[-1]
    count = width // 4
    half = width // 2
    freqs = theta ** (-jnp.arange(count, dtype=jnp.float32) / count)
    extra = (1,) * (vector.ndim - 2)
    pieces = []
    for portion, shift in ((vector[..., :half], row_shift), (vector[..., half:], col_shift)):
        angle = (shift.astype(jnp.float32)[:, None] * freqs[None, :]).reshape(
            (shift.shape[0],) + extra + (count,)
        )
        lower = portion[..., :count]
        upper = portion[..., count:]
        pieces.append(
            jnp.concatenate(
                [
                    lower * jnp.cos(angle) - upper * jnp.sin(angle),
                    lower * jnp.sin(angle) + upper * jnp.cos(angle),
                ],
                axis=-1,
            )
        )
    return jnp.concatenate(pieces, axis=-1)


def norm_scale(values, gain):
    wide = values.astype(jnp.float32)
    return (
        wide
        * lax.rsqrt(jnp.mean(wide * wide, axis=-1, keepdims=True) + eps)
        * gain.astype(jnp.float32)
    )


def expert_active(rows, gate_w, up_w):
    gate_pre = jnp.minimum(jnp.dot(rows, gate_w, preferred_element_type=jnp.float32), limit)
    up_pre = jnp.clip(jnp.dot(rows, up_w, preferred_element_type=jnp.float32), -limit, limit)
    return ((up_pre + 1.0) * gate_pre * jax.nn.sigmoid(slope * gate_pre)).astype(jnp.bfloat16)


def on_device(
    query_plain,
    query_turn,
    latent,
    key_turn,
    latent_norm_scale,
    plain_key_matrix,
    value_matrix,
    residual,
    out_weight,
    ffn_gain,
    gate_weight,
    up_weight,
    down_weight,
    routes,
    route_weights,
):
    tok_dev = latent.shape[0]
    heads_dev = query_plain.shape[1] // PLAIN_HEAD_WIDTH
    model_width = residual.shape[1]
    place = lax.axis_index("sp") * tok_dev + jnp.arange(tok_dev, dtype=jnp.int32)
    grid_row = place // GRID_W
    grid_col = place % GRID_W
    normed_latent = norm_scale(latent, latent_norm_scale).astype(jnp.bfloat16)
    key_rot = turn(key_turn.astype(jnp.float32), grid_row, grid_col).astype(jnp.bfloat16)
    expert_ids = jnp.arange(lax.axis_size("sp"), dtype=jnp.int32)
    share = jnp.sum(
        route_weights[..., None] * (routes[..., None] == expert_ids).astype(jnp.float32), axis=1
    )
    latent_width = latent.shape[1]
    sent = jnp.concatenate([normed_latent, key_rot], axis=1)
    everyone = lax.all_gather(sent, "sp", axis=0, tiled=True)
    shares = lax.all_gather(share, ("sp", "tp"), axis=0, tiled=True)
    all_latent = everyone[:, :latent_width]
    all_rot = everyone[:, latent_width:]
    keys = jnp.dot(all_latent, plain_key_matrix, preferred_element_type=jnp.float32).astype(
        jnp.bfloat16
    )
    values = jnp.dot(all_latent, value_matrix, preferred_element_type=jnp.float32).astype(
        jnp.bfloat16
    )
    query_rot = turn(
        query_turn.astype(jnp.float32).reshape(tok_dev, heads_dev, QK_ROPE), grid_row, grid_col
    ).astype(jnp.bfloat16)
    scale = (PLAIN_HEAD_WIDTH + QK_ROPE) ** (-0.5)
    attended = []
    for head in range(heads_dev):
        span = slice(head * PLAIN_HEAD_WIDTH, (head + 1) * PLAIN_HEAD_WIDTH)
        scores = (
            jnp.einsum(
                "qd,kd->qk", query_plain[:, span], keys[:, span], preferred_element_type=jnp.float32
            )
            + jnp.einsum(
                "qd,kd->qk", query_rot[:, head], all_rot, preferred_element_type=jnp.float32
            )
        ) * scale
        weights = jnp.exp(scores - jnp.max(scores, axis=1, keepdims=True))
        summed = jnp.dot(
            weights.astype(jnp.bfloat16),
            values[:, head * VALUE_WIDTH : (head + 1) * VALUE_WIDTH],
            preferred_element_type=jnp.float32,
        )
        attended.append(
            (summed / jnp.sum(weights, axis=1, keepdims=True)).astype(jnp.bfloat16)
        )
    attended = jnp.concatenate(attended, axis=1)
    rows_dev = residual.shape[0]
    group = lax.axis_size("tp")
    swapped = lax.all_to_all(
        attended.reshape(group, rows_dev, heads_dev * VALUE_WIDTH),
        "tp",
        split_axis=0,
        concat_axis=0,
        tiled=True,
    )
    own_rows = jnp.transpose(swapped, (1, 0, 2)).reshape(rows_dev, group * heads_dev * VALUE_WIDTH)
    projected = jnp.dot(own_rows, out_weight, preferred_element_type=jnp.float32)
    hidden = (residual.astype(jnp.float32) + projected).astype(jnp.bfloat16)
    normed = norm_scale(hidden, ffn_gain).astype(jnp.bfloat16)
    rows = lax.all_gather(normed, ("sp", "tp"), axis=0, tiled=True)
    active = expert_active(rows, gate_weight[0], up_weight[0])
    product = jnp.dot(active, down_weight[0], preferred_element_type=jnp.float32)
    own_share = jnp.sum(
        jnp.where(expert_ids[None, :] == lax.axis_index("sp"), shares, 0.0), axis=1, keepdims=True
    )
    mixture = lax.psum_scatter(
        (own_share * product).astype(jnp.bfloat16),
        ("sp", "tp"),
        scatter_dimension=0,
        tiled=True,
    )
    return (hidden.astype(jnp.float32) + mixture.astype(jnp.float32)).astype(jnp.bfloat16)


def solution(mesh):
    placed = (
        P(("grp", "sp"), "tp"),
        P(("grp", "sp"), "tp"),
        P(("grp", "sp"), None),
        P(("grp", "sp"), None),
        P(),
        P(None, "tp"),
        P(None, "tp"),
        P(("grp", "sp", "tp"), None),
        P(),
        P(),
        P("sp", None, "tp"),
        P("sp", None, "tp"),
        P("sp", "tp", None),
        P(("grp", "sp", "tp"), None),
        P(("grp", "sp", "tp"), None),
    )
    return jax.shard_map(
        on_device,
        mesh=mesh,
        in_specs=placed,
        out_specs=P(("grp", "sp", "tp"), None),
        check_vma=False,
    )
```

```python
import functools

import jax
import jax.numpy as jnp
from jax import lax
from jax.experimental import pallas as pl
from jax.experimental.pallas import tpu as pltpu
from jax.sharding import PartitionSpec as P

PLAIN_HEAD_WIDTH = 128
QK_ROPE = 64
VALUE_WIDTH = 128
GRID_W = 64


theta = 10000.0
eps = 1e-06
limit = 7.0
slope = 1.702
CORES = 2
VMEM_BYTES = 60 * 2**20


def turn(vector, row_shift, col_shift):
    width = vector.shape[-1]
    count = width // 4
    half = width // 2
    freqs = theta ** (-jnp.arange(count, dtype=jnp.float32) / count)
    extra = (1,) * (vector.ndim - 2)
    pieces = []
    for portion, shift in ((vector[..., :half], row_shift), (vector[..., half:], col_shift)):
        angle = (shift.astype(jnp.float32)[:, None] * freqs[None, :]).reshape(
            (shift.shape[0],) + extra + (count,)
        )
        lower = portion[..., :count]
        upper = portion[..., count:]
        pieces.append(
            jnp.concatenate(
                [
                    lower * jnp.cos(angle) - upper * jnp.sin(angle),
                    lower * jnp.sin(angle) + upper * jnp.cos(angle),
                ],
                axis=-1,
            )
        )
    return jnp.concatenate(pieces, axis=-1)


def norm_scale(values, gain):
    wide = values.astype(jnp.float32)
    return (
        wide
        * lax.rsqrt(jnp.mean(wide * wide, axis=-1, keepdims=True) + eps)
        * gain.astype(jnp.float32)
    )


def expert_active(rows, gate_w, up_w):
    gate_pre = jnp.minimum(jnp.dot(rows, gate_w, preferred_element_type=jnp.float32), limit)
    up_pre = jnp.clip(jnp.dot(rows, up_w, preferred_element_type=jnp.float32), -limit, limit)
    return ((up_pre + 1.0) * gate_pre * jax.nn.sigmoid(slope * gate_pre)).astype(jnp.bfloat16)


def flipped(index, mask):
    out = index
    bit = 1
    while bit <= mask:
        if mask & bit:
            out = out + bit - 2 * bit * ((index // bit) % 2)
        bit *= 2
    return out


def experts_kernel(
    chips,
    group,
    rows_ref,
    hidden_ref,
    share_ref,
    gate_hbm,
    up_hbm,
    down_hbm,
    out_ref,
    gathered,
    partial,
    from_core,
    from_tp,
    from_chip,
    gate_ref,
    up_ref,
    down_ref,
    load_sem,
    z_send,
    z_recv,
    x_send,
    x_recv,
    c_send,
    c_recv,
    rc_send,
    rc_recv,
    rx_send,
    rx_recv,
    rz_send,
    rz_recv,
):
    place = lax.axis_index("sp")
    column = lax.axis_index("tp")
    chip, core = place // CORES, place % CORES
    rows_dev, model_width = rows_ref.shape
    per_chip = CORES * group

    def other(index, shift):
        return (index + shift) % group

    def slot(k, core_at, column_at):
        return flipped(chip, k) * per_chip + core_at * group + column_at

    partner = {"sp": chip * CORES + 1 - core}

    def chip_peer(k):
        return {"sp": flipped(chip, k) * CORES + core}

    barrier = pltpu.get_barrier_semaphore()
    pl.semaphore_signal(barrier, inc=1, device_id=partner)
    for k in range(1, chips):
        pl.semaphore_signal(barrier, inc=1, device_id=chip_peer(k))
    for shift in range(1, group):
        pl.semaphore_signal(barrier, inc=1, device_id={"tp": other(column, shift)})
    loads = [
        pltpu.make_async_copy(src, dst, load_sem.at[i])
        for i, (src, dst) in enumerate(
            ((gate_hbm, gate_ref), (up_hbm, up_ref), (down_hbm, down_ref))
        )
    ]
    for load in loads:
        load.start()
    pl.semaphore_wait(barrier, chips + group - 1)

    sends = []

    def remote(src, dst, send_sem, recv_sem, device):
        return pltpu.make_async_remote_copy(
            src_ref=src, dst_ref=dst, send_sem=send_sem, recv_sem=recv_sem, device_id=device
        )

    def launch(copy):
        copy.start()
        sends.append(copy)

    def source(k, back):
        if k == 0 and back == 0:
            return rows_ref
        return gathered.at[slot(k, core, other(column, group - back))]

    def chip_copy(k):
        return remote(
            rows_ref, gathered.at[slot(0, core, column)], z_send.at[k], z_recv.at[k], chip_peer(k)
        )

    def chip_wait(k):
        landed = gathered.at[slot(k, core, column)]
        remote(landed, landed, z_send.at[k], z_recv.at[k], chip_peer(k)).wait_recv()

    def tp_copy(k, shift):
        return remote(
            source(k, 0),
            gathered.at[slot(k, core, column)],
            x_send.at[k, shift],
            x_recv.at[k, shift],
            {"tp": other(column, shift)},
        )

    def tp_wait(k, shift):
        landed = gathered.at[slot(k, core, other(column, group - shift))]
        remote(
            landed,
            landed,
            x_send.at[k, shift],
            x_recv.at[k, shift],
            {"tp": other(column, shift)},
        ).wait_recv()

    def core_copy(k, back):
        return remote(
            source(k, back),
            gathered.at[slot(k, core, other(column, group - back))],
            c_send.at[k, back],
            c_recv.at[k, back],
            partner,
        )

    def core_wait(k, back):
        landed = gathered.at[slot(k, 1 - core, other(column, group - back))]
        remote(landed, landed, c_send.at[k, back], c_recv.at[k, back], partner).wait_recv()

    def spread(k):
        for shift in range(1, group):
            launch(tp_copy(k, shift))
        launch(core_copy(k, 0))

    def compute(k):
        first = flipped(chip, k) * per_chip
        rows = gathered[pl.ds(first, per_chip)].reshape(per_chip * rows_dev, model_width)
        active = expert_active(rows, gate_ref[...], up_ref[...])
        share = share_ref[pl.ds(first, per_chip)].reshape(per_chip * rows_dev, 1)
        product = jnp.dot(active, down_ref[...], preferred_element_type=jnp.float32)
        partial[pl.ds(first, per_chip)] = (
            (product * share).astype(jnp.bfloat16).reshape(per_chip, rows_dev, model_width)
        )

    def partner_copy(k):
        return remote(
            partial.at[pl.ds(slot(k, 1 - core, 0), group)],
            from_core.at[k],
            rc_send.at[k],
            rc_recv.at[k],
            partner,
        )

    def sum_cores(k):
        partner_copy(k).wait_recv()
        first = slot(k, core, 0)
        partial[pl.ds(first, group)] = (
            partial[pl.ds(first, group)].astype(jnp.float32) + from_core[k].astype(jnp.float32)
        ).astype(jnp.bfloat16)
        for shift in range(1, group):
            launch(tp_sum_copy(k, shift))

    def tp_sum_copy(k, shift):
        return remote(
            partial.at[slot(k, core, other(column, shift))],
            from_tp.at[k, shift - 1],
            rx_send.at[k, shift],
            rx_recv.at[k, shift],
            {"tp": other(column, shift)},
        )

    def chip_sum_copy(k):
        return remote(
            partial.at[slot(k, core, column)],
            from_chip.at[k],
            rz_send.at[k],
            rz_recv.at[k],
            chip_peer(k),
        )

    def sum_tp(k):
        total = partial[slot(k, core, column)].astype(jnp.float32)
        for shift in range(1, group):
            tp_sum_copy(k, shift).wait_recv()
            total = total + from_tp[k, shift - 1].astype(jnp.float32)
        if k == 0:
            out_ref[...] = (hidden_ref[...].astype(jnp.float32) + total)
            return
        partial[slot(k, core, column)] = total.astype(jnp.bfloat16)
        launch(chip_sum_copy(k))

    spread(0)
    for k in range(1, chips):
        launch(chip_copy(k))
    gathered[slot(0, core, column)] = rows_ref[...]
    for k in range(chips + 2):
        if k < chips:
            for shift in range(1, group):
                tp_wait(k, shift)
                launch(core_copy(k, shift))
            if k + 1 < chips:
                chip_wait(k + 1)
                spread(k + 1)
            for back in range(group):
                core_wait(k, back)
            if k == 0:
                for load in loads:
                    load.wait()
            compute(k)
            launch(partner_copy(k))
        if 0 <= k - 1 < chips:
            sum_cores(k - 1)
        if 0 <= k - 2 < chips:
            sum_tp(k - 2)
    for k in range(1, chips):
        chip_sum_copy(k).wait_recv()
        out_ref[...] += from_chip[k].astype(jnp.float32)
    for copy in sends:
        copy.wait_send()


def run_experts(rows, hidden, shares, gate_w, up_w, down_w):
    group = lax.axis_size("tp")
    chips = lax.axis_size("sp") // CORES
    rows_dev, model_width = rows.shape
    blocks = chips * CORES * group
    dma = pltpu.SemaphoreType.DMA
    block = (rows_dev, model_width)
    whole = pl.BlockSpec(memory_space=pltpu.VMEM)
    return pl.pallas_call(
        functools.partial(experts_kernel, chips, group),
        out_shape=jax.ShapeDtypeStruct(block, jnp.float32),
        in_specs=[whole] * 3 + [pl.BlockSpec(memory_space=pl.ANY)] * 3,
        out_specs=whole,
        scratch_shapes=[
            pltpu.VMEM((blocks,) + block, jnp.bfloat16),
            pltpu.VMEM((blocks,) + block, jnp.bfloat16),
            pltpu.VMEM((chips, group) + block, jnp.bfloat16),
            pltpu.VMEM((chips, group - 1) + block, jnp.bfloat16),
            pltpu.VMEM((chips,) + block, jnp.bfloat16),
            pltpu.VMEM(gate_w.shape, jnp.bfloat16),
            pltpu.VMEM(up_w.shape, jnp.bfloat16),
            pltpu.VMEM(down_w.shape, jnp.bfloat16),
            dma((3,)),
            dma((chips,)),
            dma((chips,)),
            dma((chips, group)),
            dma((chips, group)),
            dma((chips, group)),
            dma((chips, group)),
            dma((chips,)),
            dma((chips,)),
            dma((chips, group)),
            dma((chips, group)),
            dma((chips,)),
            dma((chips,)),
        ],
        compiler_params=pltpu.CompilerParams(
            collective_id=0, has_side_effects=True, vmem_limit_bytes=VMEM_BYTES
        ),
    )(rows, hidden, shares.reshape(blocks, rows_dev, 1), gate_w, up_w, down_w)


def experts_fit(rows_dev, model_width):
    group, places = lax.axis_size("tp"), lax.axis_size("sp")
    chips = places // CORES
    if group < 2 or places % CORES or chips & (chips - 1) or rows_dev % 16:
        return False
    return 3 * places * group * rows_dev * model_width * 2 < VMEM_BYTES // 2


def on_device(
    query_plain,
    query_turn,
    latent,
    key_turn,
    latent_norm_scale,
    plain_key_matrix,
    value_matrix,
    residual,
    out_weight,
    ffn_gain,
    gate_weight,
    up_weight,
    down_weight,
    routes,
    route_weights,
):
    tok_dev = latent.shape[0]
    heads_dev = query_plain.shape[1] // PLAIN_HEAD_WIDTH
    model_width = residual.shape[1]
    place = lax.axis_index("sp") * tok_dev + jnp.arange(tok_dev, dtype=jnp.int32)
    grid_row = place // GRID_W
    grid_col = place % GRID_W
    normed_latent = norm_scale(latent, latent_norm_scale).astype(jnp.bfloat16)
    key_rot = turn(key_turn.astype(jnp.float32), grid_row, grid_col).astype(jnp.bfloat16)
    expert_ids = jnp.arange(lax.axis_size("sp"), dtype=jnp.int32)
    share = jnp.sum(
        route_weights[..., None] * (routes[..., None] == expert_ids).astype(jnp.float32), axis=1
    )
    latent_width = latent.shape[1]
    sent = jnp.concatenate([normed_latent, key_rot], axis=1)
    everyone = lax.all_gather(sent, "sp", axis=0, tiled=True)
    shares = lax.all_gather(share, ("sp", "tp"), axis=0, tiled=True)
    all_latent = everyone[:, :latent_width]
    all_rot = everyone[:, latent_width:]
    keys = jnp.dot(all_latent, plain_key_matrix, preferred_element_type=jnp.float32).astype(
        jnp.bfloat16
    )
    values = jnp.dot(all_latent, value_matrix, preferred_element_type=jnp.float32).astype(
        jnp.bfloat16
    )
    query_rot = turn(
        query_turn.astype(jnp.float32).reshape(tok_dev, heads_dev, QK_ROPE), grid_row, grid_col
    ).astype(jnp.bfloat16)
    scale = (PLAIN_HEAD_WIDTH + QK_ROPE) ** (-0.5)
    attended = []
    for head in range(heads_dev):
        span = slice(head * PLAIN_HEAD_WIDTH, (head + 1) * PLAIN_HEAD_WIDTH)
        scores = (
            jnp.einsum(
                "qd,kd->qk", query_plain[:, span], keys[:, span], preferred_element_type=jnp.float32
            )
            + jnp.einsum(
                "qd,kd->qk", query_rot[:, head], all_rot, preferred_element_type=jnp.float32
            )
        ) * scale
        weights = jnp.exp(scores - jnp.max(scores, axis=1, keepdims=True))
        summed = jnp.dot(
            weights.astype(jnp.bfloat16),
            values[:, head * VALUE_WIDTH : (head + 1) * VALUE_WIDTH],
            preferred_element_type=jnp.float32,
        )
        attended.append(
            (summed / jnp.sum(weights, axis=1, keepdims=True)).astype(jnp.bfloat16)
        )
    attended = jnp.concatenate(attended, axis=1)
    rows_dev = residual.shape[0]
    group = lax.axis_size("tp")
    swapped = lax.all_to_all(
        attended.reshape(group, rows_dev, heads_dev * VALUE_WIDTH),
        "tp",
        split_axis=0,
        concat_axis=0,
        tiled=True,
    )
    own_rows = jnp.transpose(swapped, (1, 0, 2)).reshape(rows_dev, group * heads_dev * VALUE_WIDTH)
    projected = jnp.dot(own_rows, out_weight, preferred_element_type=jnp.float32)
    hidden = (residual.astype(jnp.float32) + projected).astype(jnp.bfloat16)
    normed = norm_scale(hidden, ffn_gain).astype(jnp.bfloat16)
    own_share = jnp.sum(
        jnp.where(expert_ids[None, :] == lax.axis_index("sp"), shares, 0.0), axis=1, keepdims=True
    )
    if experts_fit(rows_dev, residual.shape[1]):
        return run_experts(
            normed, hidden, own_share, gate_weight[0], up_weight[0], down_weight[0]
        ).astype(jnp.bfloat16)
    rows = lax.all_gather(normed, ("sp", "tp"), axis=0, tiled=True)
    active = expert_active(rows, gate_weight[0], up_weight[0])
    product = jnp.dot(active, down_weight[0], preferred_element_type=jnp.float32)
    mixture = lax.psum_scatter(
        (own_share * product).astype(jnp.bfloat16),
        ("sp", "tp"),
        scatter_dimension=0,
        tiled=True,
    )
    return (hidden.astype(jnp.float32) + mixture.astype(jnp.float32)).astype(jnp.bfloat16)


def solution(mesh):
    placed = (
        P(("grp", "sp"), "tp"),
        P(("grp", "sp"), "tp"),
        P(("grp", "sp"), None),
        P(("grp", "sp"), None),
        P(),
        P(None, "tp"),
        P(None, "tp"),
        P(("grp", "sp", "tp"), None),
        P(),
        P(),
        P("sp", None, "tp"),
        P("sp", None, "tp"),
        P("sp", "tp", None),
        P(("grp", "sp", "tp"), None),
        P(("grp", "sp", "tp"), None),
    )
    return jax.shard_map(
        on_device,
        mesh=mesh,
        in_specs=placed,
        out_specs=P(("grp", "sp", "tp"), None),
        check_vma=False,
    )
```

```python
import functools

import jax
import jax.numpy as jnp
from jax import lax
from jax.experimental import pallas as pl
from jax.experimental.pallas import tpu as pltpu
from jax.sharding import PartitionSpec as P

PLAIN_HEAD_WIDTH = 128
QK_ROPE = 64
VALUE_WIDTH = 128
GRID_W = 64


theta = 10000.0
eps = 1e-06
limit = 7.0
slope = 1.702
CORES = 2
VMEM_BYTES = 60 * 2**20


def turn(vector, row_shift, col_shift):
    width = vector.shape[-1]
    count = width // 4
    half = width // 2
    freqs = theta ** (-jnp.arange(count, dtype=jnp.float32) / count)
    extra = (1,) * (vector.ndim - 2)
    pieces = []
    for portion, shift in ((vector[..., :half], row_shift), (vector[..., half:], col_shift)):
        angle = (shift.astype(jnp.float32)[:, None] * freqs[None, :]).reshape(
            (shift.shape[0],) + extra + (count,)
        )
        lower = portion[..., :count]
        upper = portion[..., count:]
        pieces.append(
            jnp.concatenate(
                [
                    lower * jnp.cos(angle) - upper * jnp.sin(angle),
                    lower * jnp.sin(angle) + upper * jnp.cos(angle),
                ],
                axis=-1,
            )
        )
    return jnp.concatenate(pieces, axis=-1)


def norm_scale(values, gain):
    wide = values.astype(jnp.float32)
    return (
        wide
        * lax.rsqrt(jnp.mean(wide * wide, axis=-1, keepdims=True) + eps)
        * gain.astype(jnp.float32)
    )


def expert_active(rows, gate_w, up_w):
    gate_pre = jnp.minimum(jnp.dot(rows, gate_w, preferred_element_type=jnp.float32), limit)
    up_pre = jnp.clip(jnp.dot(rows, up_w, preferred_element_type=jnp.float32), -limit, limit)
    return ((up_pre + 1.0) * gate_pre * jax.nn.sigmoid(slope * gate_pre)).astype(jnp.bfloat16)


def flipped(index, mask):
    out = index
    bit = 1
    while bit <= mask:
        if mask & bit:
            out = out + bit - 2 * bit * ((index // bit) % 2)
        bit *= 2
    return out


def gatherer(chips, group, own, gathered, sems, launch):
    z_send, z_recv, x_send, x_recv, c_send, c_recv = sems
    place = lax.axis_index("sp")
    column = lax.axis_index("tp")
    chip, core = place // CORES, place % CORES
    per_chip = CORES * group
    partner = {"sp": chip * CORES + 1 - core}

    def other(shift):
        return (column + shift) % group

    def slot(k, core_at, column_at):
        return flipped(chip, k) * per_chip + core_at * group + column_at

    def chip_peer(k):
        return {"sp": flipped(chip, k) * CORES + core}

    def remote(src, dst, send_sem, recv_sem, device):
        return pltpu.make_async_remote_copy(
            src_ref=src, dst_ref=dst, send_sem=send_sem, recv_sem=recv_sem, device_id=device
        )

    def greet():
        barrier = pltpu.get_barrier_semaphore()
        pl.semaphore_signal(barrier, inc=1, device_id=partner)
        for k in range(1, chips):
            pl.semaphore_signal(barrier, inc=1, device_id=chip_peer(k))
        for shift in range(1, group):
            pl.semaphore_signal(barrier, inc=1, device_id={"tp": other(shift)})

    def met():
        pl.semaphore_wait(pltpu.get_barrier_semaphore(), chips + group - 1)

    def source(k, back):
        if k == 0 and back == 0:
            return own
        return gathered.at[slot(k, core, other(group - back))]

    def chip_wait(k):
        landed = gathered.at[slot(k, core, column)]
        remote(landed, landed, z_send.at[k], z_recv.at[k], chip_peer(k)).wait_recv()

    def core_copy(k, back):
        return remote(
            source(k, back),
            gathered.at[slot(k, core, other(group - back))],
            c_send.at[k, back],
            c_recv.at[k, back],
            partner,
        )

    def core_wait(k, back):
        landed = gathered.at[slot(k, 1 - core, other(group - back))]
        remote(landed, landed, c_send.at[k, back], c_recv.at[k, back], partner).wait_recv()

    def tp_copy(k, shift):
        return remote(
            source(k, 0),
            gathered.at[slot(k, core, column)],
            x_send.at[k, shift],
            x_recv.at[k, shift],
            {"tp": other(shift)},
        )

    def tp_wait(k, shift):
        landed = gathered.at[slot(k, core, other(group - shift))]
        remote(
            landed, landed, x_send.at[k, shift], x_recv.at[k, shift], {"tp": other(shift)}
        ).wait_recv()

    def spread(k):
        for shift in range(1, group):
            launch(tp_copy(k, shift))
        launch(core_copy(k, 0))

    def begin():
        for k in range(1, chips):
            launch(
                remote(
                    own,
                    gathered.at[slot(0, core, column)],
                    z_send.at[k],
                    z_recv.at[k],
                    chip_peer(k),
                )
            )
        spread(0)

    def step(k):
        for shift in range(1, group):
            tp_wait(k, shift)
            launch(core_copy(k, shift))
        if k + 1 < chips:
            chip_wait(k + 1)
            spread(k + 1)
        for back in range(group):
            core_wait(k, back)

    return greet, met, begin, step, slot, chip_peer, partner, other, remote


def gather_kernel(chips, group, own, gathered, *sems):
    sends = []

    def launch(copy):
        copy.start()
        sends.append(copy)

    greet, met, begin, step, slot = gatherer(chips, group, own, gathered, sems, launch)[:5]
    greet()
    met()
    begin()
    gathered[slot(0, lax.axis_index("sp") % CORES, lax.axis_index("tp"))] = own[...]
    for k in range(chips):
        step(k)
    for copy in sends:
        copy.wait_send()


def gather_sems(chips, group):
    dma = pltpu.SemaphoreType.DMA
    return [dma((chips,))] * 2 + [dma((chips, group))] * 4


def run_gather(rows):
    group = lax.axis_size("tp")
    chips = lax.axis_size("sp") // CORES
    whole = pl.BlockSpec(memory_space=pltpu.VMEM)
    return pl.pallas_call(
        functools.partial(gather_kernel, chips, group),
        out_shape=jax.ShapeDtypeStruct((chips * CORES * group,) + rows.shape, rows.dtype),
        in_specs=[whole],
        out_specs=whole,
        scratch_shapes=gather_sems(chips, group),
        compiler_params=pltpu.CompilerParams(
            collective_id=1, has_side_effects=True, vmem_limit_bytes=VMEM_BYTES // 2
        ),
    )(rows)


def experts_kernel(
    chips,
    group,
    attended_ref,
    residual_ref,
    gain_ref,
    share_ref,
    out_hbm,
    gate_hbm,
    up_hbm,
    down_hbm,
    out_ref,
    heads,
    hidden,
    rows_ref,
    total_ref,
    gathered,
    partial,
    from_core,
    from_tp,
    from_chip,
    outw_ref,
    gate_ref,
    up_ref,
    down_ref,
    load_sem,
    h_send,
    h_recv,
    rc_send,
    rc_recv,
    rx_send,
    rx_recv,
    rz_send,
    rz_recv,
    *sems,
):
    column = lax.axis_index("tp")
    core = lax.axis_index("sp") % CORES
    rows_dev, model_width = rows_ref.shape
    per_chip = CORES * group
    sends = []

    def launch(copy):
        copy.start()
        sends.append(copy)

    greet, met, begin, step, slot, chip_peer, partner, other, remote = gatherer(
        chips, group, rows_ref, gathered, sems, launch
    )
    greet()
    loads = [
        pltpu.make_async_copy(src, dst, load_sem.at[i])
        for i, (src, dst) in enumerate(
            (
                (out_hbm, outw_ref),
                (gate_hbm, gate_ref),
                (up_hbm, up_ref),
                (down_hbm, down_ref),
            )
        )
    ]
    for load in loads:
        load.start()
    met()

    def heads_copy(shift):
        return remote(
            attended_ref.at[other(shift)],
            heads.at[column],
            h_send.at[shift],
            h_recv.at[shift],
            {"tp": other(shift)},
        )

    def heads_wait(shift):
        landed = heads.at[other(group - shift)]
        remote(
            landed, landed, h_send.at[shift], h_recv.at[shift], {"tp": other(shift)}
        ).wait_recv()

    for shift in range(1, group):
        launch(heads_copy(shift))
    heads[column] = attended_ref[column]
    loads[0].wait()
    for shift in range(1, group):
        heads_wait(shift)
    joined = jnp.concatenate([heads[at] for at in range(group)], axis=1)
    projected = jnp.dot(joined, outw_ref[...], preferred_element_type=jnp.float32)
    mixed = (residual_ref[...].astype(jnp.float32) + projected).astype(jnp.bfloat16)
    normed = norm_scale(mixed, gain_ref[...]).astype(jnp.bfloat16)
    rows_ref[...] = normed
    gathered[slot(0, core, column)] = normed
    hidden[...] = mixed
    begin()

    def compute(k):
        first = slot(k, 0, 0)
        rows = gathered[pl.ds(first, per_chip)].reshape(per_chip * rows_dev, model_width)
        active = expert_active(rows, gate_ref[...], up_ref[...])
        share = share_ref[pl.ds(first, per_chip)].reshape(per_chip * rows_dev, 1)
        product = jnp.dot(active, down_ref[...], preferred_element_type=jnp.float32)
        partial[pl.ds(first, per_chip)] = (
            (product * share).astype(jnp.bfloat16).reshape(per_chip, rows_dev, model_width)
        )

    def partner_copy(k):
        return remote(
            partial.at[pl.ds(slot(k, 1 - core, 0), group)],
            from_core.at[k],
            rc_send.at[k],
            rc_recv.at[k],
            partner,
        )

    def tp_sum_copy(k, shift):
        return remote(
            partial.at[slot(k, core, other(shift))],
            from_tp.at[k, shift - 1],
            rx_send.at[k, shift],
            rx_recv.at[k, shift],
            {"tp": other(shift)},
        )

    def chip_sum_copy(k):
        return remote(
            partial.at[slot(k, core, column)],
            from_chip.at[k],
            rz_send.at[k],
            rz_recv.at[k],
            chip_peer(k),
        )

    def sum_cores(k):
        partner_copy(k).wait_recv()
        first = slot(k, core, 0)
        partial[pl.ds(first, group)] = (
            partial[pl.ds(first, group)].astype(jnp.float32) + from_core[k].astype(jnp.float32)
        ).astype(jnp.bfloat16)
        for shift in range(1, group):
            launch(tp_sum_copy(k, shift))

    def sum_tp(k):
        total = partial[slot(k, core, column)].astype(jnp.float32)
        for shift in range(1, group):
            tp_sum_copy(k, shift).wait_recv()
            total = total + from_tp[k, shift - 1].astype(jnp.float32)
        if k == 0:
            total_ref[...] = hidden[...].astype(jnp.float32) + total
            return
        partial[slot(k, core, column)] = total.astype(jnp.bfloat16)
        launch(chip_sum_copy(k))

    for k in range(chips + 2):
        if k < chips:
            step(k)
            if k == 0:
                for load in loads[1:]:
                    load.wait()
            compute(k)
            launch(partner_copy(k))
        if 0 <= k - 1 < chips:
            sum_cores(k - 1)
        if 0 <= k - 2 < chips:
            sum_tp(k - 2)
    total = total_ref[...]
    for k in range(1, chips):
        chip_sum_copy(k).wait_recv()
        total = total + from_chip[k].astype(jnp.float32)
    out_ref[...] = total.astype(jnp.bfloat16)
    for copy in sends:
        copy.wait_send()


def run_experts(attended, residual, gain, shares, out_w, gate_w, up_w, down_w):
    group = lax.axis_size("tp")
    chips = lax.axis_size("sp") // CORES
    rows_dev, model_width = residual.shape
    blocks = chips * CORES * group
    dma = pltpu.SemaphoreType.DMA
    block = (rows_dev, model_width)
    heads = (group, rows_dev, attended.shape[1])
    whole = pl.BlockSpec(memory_space=pltpu.VMEM)
    return pl.pallas_call(
        functools.partial(experts_kernel, chips, group),
        out_shape=jax.ShapeDtypeStruct(block, jnp.bfloat16),
        in_specs=[whole] * 4 + [pl.BlockSpec(memory_space=pl.ANY)] * 4,
        out_specs=whole,
        scratch_shapes=[
            pltpu.VMEM(heads, jnp.bfloat16),
            pltpu.VMEM(block, jnp.bfloat16),
            pltpu.VMEM(block, jnp.bfloat16),
            pltpu.VMEM(block, jnp.float32),
            pltpu.VMEM((blocks,) + block, jnp.bfloat16),
            pltpu.VMEM((blocks,) + block, jnp.bfloat16),
            pltpu.VMEM((chips, group) + block, jnp.bfloat16),
            pltpu.VMEM((chips, group - 1) + block, jnp.bfloat16),
            pltpu.VMEM((chips,) + block, jnp.bfloat16),
            pltpu.VMEM(out_w.shape, jnp.bfloat16),
            pltpu.VMEM(gate_w.shape, jnp.bfloat16),
            pltpu.VMEM(up_w.shape, jnp.bfloat16),
            pltpu.VMEM(down_w.shape, jnp.bfloat16),
            dma((4,)),
            dma((group,)),
            dma((group,)),
            dma((chips,)),
            dma((chips,)),
            dma((chips, group)),
            dma((chips, group)),
            dma((chips,)),
            dma((chips,)),
        ]
        + gather_sems(chips, group),
        compiler_params=pltpu.CompilerParams(
            collective_id=0, has_side_effects=True, vmem_limit_bytes=VMEM_BYTES
        ),
    )(
        attended.reshape(heads),
        residual,
        gain.reshape(1, model_width),
        shares.reshape(blocks, rows_dev, 1),
        out_w,
        gate_w,
        up_w,
        down_w,
    )


def experts_fit(rows_dev, model_width):
    group, places = lax.axis_size("tp"), lax.axis_size("sp")
    chips = places // CORES
    if group < 2 or places % CORES or chips & (chips - 1) or rows_dev % 16:
        return False
    return 3 * places * group * rows_dev * model_width * 2 < VMEM_BYTES // 2


def on_device(
    query_plain,
    query_turn,
    latent,
    key_turn,
    latent_norm_scale,
    plain_key_matrix,
    value_matrix,
    residual,
    out_weight,
    ffn_gain,
    gate_weight,
    up_weight,
    down_weight,
    routes,
    route_weights,
):
    tok_dev = latent.shape[0]
    heads_dev = query_plain.shape[1] // PLAIN_HEAD_WIDTH
    model_width = residual.shape[1]
    place = lax.axis_index("sp") * tok_dev + jnp.arange(tok_dev, dtype=jnp.int32)
    grid_row = place // GRID_W
    grid_col = place % GRID_W
    rows_dev, model_width = residual.shape
    group = lax.axis_size("tp")
    count = lax.axis_size("sp")
    fits = experts_fit(rows_dev, model_width)
    expert_ids = jnp.arange(count, dtype=jnp.int32)
    share = jnp.sum(
        route_weights[..., None] * (routes[..., None] == expert_ids).astype(jnp.float32), axis=1
    )
    latent_width = latent.shape[1]
    wide = latent_width + QK_ROPE

    def key_side(latents, turns, at_row, at_col):
        normed_latent = norm_scale(latents, latent_norm_scale).astype(jnp.bfloat16)
        key_rot = turn(turns.astype(jnp.float32), at_row, at_col).astype(jnp.bfloat16)
        return [normed_latent, key_rot]

    if fits:
        first = lax.axis_index("tp") * rows_dev
        high = lax.reduce_precision(share, 8, 7)
        filled = wide + 2 * count
        sent = jnp.concatenate(
            key_side(
                lax.dynamic_slice_in_dim(latent, first, rows_dev, 0),
                lax.dynamic_slice_in_dim(key_turn, first, rows_dev, 0),
                lax.dynamic_slice_in_dim(grid_row, first, rows_dev, 0),
                lax.dynamic_slice_in_dim(grid_col, first, rows_dev, 0),
            )
            + [high.astype(jnp.bfloat16), (share - high).astype(jnp.bfloat16)]
            + [jnp.zeros((rows_dev, -filled % 128), jnp.bfloat16)],
            axis=1,
        )
        everyone = run_gather(sent)
        everyone = everyone.reshape(everyone.shape[0] * rows_dev, everyone.shape[2])
        shares = everyone[:, wide : wide + count].astype(jnp.float32) + everyone[
            :, wide + count : filled
        ].astype(jnp.float32)
    else:
        sent = jnp.concatenate(key_side(latent, key_turn, grid_row, grid_col), axis=1)
        everyone = lax.all_gather(sent, "sp", axis=0, tiled=True)
        shares = lax.all_gather(share, ("sp", "tp"), axis=0, tiled=True)
    own_share = jnp.sum(
        jnp.where(expert_ids[None, :] == lax.axis_index("sp"), shares, 0.0), axis=1, keepdims=True
    )
    all_latent = everyone[:, :latent_width]
    all_rot = everyone[:, latent_width:wide]
    keys = jnp.dot(all_latent, plain_key_matrix, preferred_element_type=jnp.float32).astype(
        jnp.bfloat16
    )
    values = jnp.dot(all_latent, value_matrix, preferred_element_type=jnp.float32).astype(
        jnp.bfloat16
    )
    query_rot = turn(
        query_turn.astype(jnp.float32).reshape(tok_dev, heads_dev, QK_ROPE), grid_row, grid_col
    ).astype(jnp.bfloat16)
    scale = (PLAIN_HEAD_WIDTH + QK_ROPE) ** (-0.5)
    attended = []
    for head in range(heads_dev):
        span = slice(head * PLAIN_HEAD_WIDTH, (head + 1) * PLAIN_HEAD_WIDTH)
        scores = (
            jnp.einsum(
                "qd,kd->qk", query_plain[:, span], keys[:, span], preferred_element_type=jnp.float32
            )
            + jnp.einsum(
                "qd,kd->qk", query_rot[:, head], all_rot, preferred_element_type=jnp.float32
            )
        ) * scale
        weights = jnp.exp(scores - jnp.max(scores, axis=1, keepdims=True))
        summed = jnp.dot(
            weights.astype(jnp.bfloat16),
            values[:, head * VALUE_WIDTH : (head + 1) * VALUE_WIDTH],
            preferred_element_type=jnp.float32,
        )
        attended.append(
            (summed / jnp.sum(weights, axis=1, keepdims=True)).astype(jnp.bfloat16)
        )
    attended = jnp.concatenate(attended, axis=1)
    if fits:
        return run_experts(
            attended,
            residual,
            ffn_gain,
            own_share,
            out_weight,
            gate_weight[0],
            up_weight[0],
            down_weight[0],
        )
    swapped = lax.all_to_all(
        attended.reshape(group, rows_dev, heads_dev * VALUE_WIDTH),
        "tp",
        split_axis=0,
        concat_axis=0,
        tiled=True,
    )
    own_rows = jnp.transpose(swapped, (1, 0, 2)).reshape(rows_dev, group * heads_dev * VALUE_WIDTH)
    projected = jnp.dot(own_rows, out_weight, preferred_element_type=jnp.float32)
    hidden = (residual.astype(jnp.float32) + projected).astype(jnp.bfloat16)
    normed = norm_scale(hidden, ffn_gain).astype(jnp.bfloat16)
    rows = lax.all_gather(normed, ("sp", "tp"), axis=0, tiled=True)
    active = expert_active(rows, gate_weight[0], up_weight[0])
    product = jnp.dot(active, down_weight[0], preferred_element_type=jnp.float32)
    mixture = lax.psum_scatter(
        (own_share * product).astype(jnp.bfloat16),
        ("sp", "tp"),
        scatter_dimension=0,
        tiled=True,
    )
    return (hidden.astype(jnp.float32) + mixture.astype(jnp.float32)).astype(jnp.bfloat16)


def solution(mesh):
    placed = (
        P(("grp", "sp"), "tp"),
        P(("grp", "sp"), "tp"),
        P(("grp", "sp"), None),
        P(("grp", "sp"), None),
        P(),
        P(None, "tp"),
        P(None, "tp"),
        P(("grp", "sp", "tp"), None),
        P(),
        P(),
        P("sp", None, "tp"),
        P("sp", None, "tp"),
        P("sp", "tp", None),
        P(("grp", "sp", "tp"), None),
        P(("grp", "sp", "tp"), None),
    )
    return jax.shard_map(
        on_device,
        mesh=mesh,
        in_specs=placed,
        out_specs=P(("grp", "sp", "tp"), None),
        check_vma=False,
    )
```
